256 devices in a mesh: grp: 2 (over y), ep: 32 (over z, core), tp: 4 (over x).
Axes of the slice: x: 4, y: 2, z: 16, core: 2. Of those that a mesh axis runs over, the one named last changes fastest.
The devices are a block of a 4x16x16 slice.
Arguments:
- tokens: bfloat16 [16384, 2048], P(('grp', 'ep', 'tp')), parts along dimension 0, may hold values from -6 to 6
- gain_in: float32 [2048], replicated, may hold values from 0.1 to 1.9
- routes: int32 [16384, 2], P(('grp', 'ep')), parts along dimension 0, may hold values from 0 to 31, all different within a row; in each aligned block of 64 rows (0 to 63, 64 to 127, ...) at most 6 rows name the same one
- gates: float32 [16384, 2], P(('grp', 'ep')), parts along dimension 0, may hold values from 0.05 to 1
- w_gate: bfloat16 [32, 2048, 3072], P('ep', None, 'tp'), may hold values from -0.125 to 0.125
- w_up: bfloat16 [32, 2048, 3072], P('ep', None, 'tp'), may hold values from -0.125 to 0.125
- w_down: bfloat16 [32, 3072, 2048], P('ep', 'tp'), may hold values from -0.109375 to 0.109375
- gain_out: float32 [2048], P('tp'), may hold values from 0.3 to 3
Outputs:
- mixed: bfloat16 [16384, 2048], P(('grp', 'ep'), 'tp'), parts along dimension 0
The draws below stay inside these ranges and needn't reach their ends.
There are 2 independent parts, one for each index of `grp`. The reference program is written for one: setup_inputs(seed, part) draws one part's arguments, and reference() takes and returns one part's arrays. A program takes and returns all parts, laid end to end along the dimension named above; an argument that names none is the same for every part. Nothing has to cross between parts.
Inputs may be any that keep to these rules, and one draw needn't show every extreme that they name: `routes`: each row names 2 different experts; every expert is named by some row. Among the rows of one device (aligned blocks of 64 rows) no expert is named more than 6 times, and in every draw some expert is named exactly 6 times in some such block.
All inputs are finite; a program needn't handle non-finite values.
Results may differ from the reference program's by a relative error of at most 0.012.
Values may be sent and summed in bfloat16 or wider, within the bound.
A program may use at most 64 MiB of HBM per device.

```python
import math
import jax
import jax.numpy as jnp
import numpy as np
from jax import lax

D = 2048
FF = 3072
TOPK = 2
TOK_DEV = 64
EXPERTS = 32
CAP = 6
FF_DEV = 768
TOKENS = 8192
N_EP = 32
N_TP = 4


def level_of(own_key, extent, split, smallest, top_value):
    level = 1.0
    for dim, blocks in split:
        heights = jax.random.uniform(jax.random.fold_in(jax.random.fold_in(own_key, 6), dim), (blocks,), jnp.float32, smallest / len(split), top_value / len(split))
        level = level * jnp.repeat(jnp.exp(heights), extent[dim] // blocks).reshape((-1,) + (1,) * (len(extent) - 1 - dim))
    return level


def deal_out(rng, own, number, rows, amount, top, reach, lean):
    sequence = jax.random.permutation(rng, amount)
    crowded, common = load_shares(amount, rows * top, reach, lean, True), load_shares(amount, rows * top, reach, lean, False)
    places = jnp.arange(amount)

    def named(tallies, turn):
        used = int((tallies > 0).sum())
        fixed = max(1, used // 4)
        passed = fixed + (places - fixed + turn * (used - fixed)) % max(1, amount - fixed)
        return jnp.zeros((amount,), jnp.int32).at[sequence[jnp.where(places < fixed, places, passed)]].set(jnp.asarray(tallies, jnp.int32))

    tallies = jnp.where(number % 4 == 0, named(crowded, number // 4), named(common, number - number // 4 - 1))
    mixed = jax.random.permutation(jax.random.fold_in(own, 3), amount)
    donor, taker = mixed[0:amount // 2 * 2:2], mixed[1:amount // 2 * 2:2]
    slack = jnp.minimum(tallies[donor] - 1, reach - tallies[taker]) // 2
    slack = jnp.where((donor == sequence[0]) | (taker == sequence[0]) | (tallies[taker] == 0), 0, jnp.maximum(slack, 0))
    passed = jax.random.randint(jax.random.fold_in(own, 4), (amount // 2,), 0, 1 << 20) % (slack + 1)
    tallies = tallies.at[donor].add(-passed).at[taker].add(passed)
    members = jnp.searchsorted(jnp.cumsum(tallies), jnp.arange(rows * top), side="right").astype(jnp.int32)
    listing = members.reshape(top, rows).T
    listing = listing[jax.random.permutation(jax.random.fold_in(own, 1), rows)]
    turn = jax.random.randint(jax.random.fold_in(own, 2), (rows, 1), 0, top)
    return jnp.take_along_axis(listing, (jnp.arange(top)[None, :] + turn) % top, axis=1)


def load_shares(number_of, total, reach, slope, full):
    portions = [(1 << 20) // math.isqrt(standing ** slope) + 1 for standing in range(1, number_of + 1)]
    largest = reach if full else min(reach, max(-(-total // number_of), total * portions[0] // sum(portions)))
    least = 1 if total - largest >= number_of - 1 else 0
    holding, spare = [largest] + [least] * (number_of - 1), total - largest - least * (number_of - 1)
    while spare > 0:
        movable = [i for i in range(1, number_of) if holding[i] < largest] or [i for i in range(1, number_of) if holding[i] < reach]
        pool, remaining = sum([portions[i] for i in movable]), spare
        for i in movable:
            extra = min(reach - holding[i], max(1, remaining * portions[i] // pool), spare)
            holding[i] = holding[i] + extra
            spare = spare - extra
    return np.array(holding)


def bell_draw(own_key, shape, scale, reach, pieces=(), held_as=jnp.bfloat16):
    values = jax.random.normal(own_key, shape, jnp.float32) * scale
    if len(pieces) > 0:
        values = level_of(own_key, shape, pieces, -0.22, 0.18) * values
    return jnp.clip(values, min=-reach, max=reach).astype(held_as)


def setup_inputs(seed: int = 0, part: int = 0) -> dict:
    streams_of = jax.random.split(jax.random.key(seed), 9)
    part_keys = jax.random.split(jax.random.fold_in(streams_of[8], part), 9)
    tokens = bell_draw(part_keys[0], (TOKENS, D), 1.0, 6.0, ((0, 128),))
    gain_in = jnp.clip(1.0 + 0.18 * jax.random.normal(streams_of[1], (D,), jnp.float32), 0.1, 1.9)
    routes_keys = jax.random.split(jax.random.fold_in(part_keys[2], 1), TOKENS // TOK_DEV)
    routes_turns = jax.random.permutation(jax.random.fold_in(part_keys[2], 3), TOKENS // TOK_DEV)
    routes = jax.vmap(lambda own, number: deal_out(jax.random.fold_in(part_keys[2], 2), own, number, TOK_DEV, EXPERTS, TOPK, CAP, 2))(routes_keys, routes_turns).reshape((TOKENS, TOPK))
    gates = jnp.clip(0.05 + 0.95 * jax.random.uniform(part_keys[3], (TOKENS, TOPK), jnp.float32) ** level_of(part_keys[3], (TOKENS, TOPK), ((0, 32),), -0.2, 0.2), 0.05, 1.0)
    w_gate = bell_draw(streams_of[4], (EXPERTS, D, FF), D ** -0.5, 0.125, ((0, 32), (2, 4)))
    w_up = bell_draw(streams_of[5], (EXPERTS, D, FF), D ** -0.5, 0.125, ((0, 32), (2, 4)))
    w_down = bell_draw(streams_of[6], (EXPERTS, FF, D), FF ** -0.5, 0.109375, ((0, 32), (1, 4)))
    gain_out = jnp.clip(jnp.exp(math.log(3.0) - 2.3025851 * jax.random.uniform(streams_of[7], (D,), jnp.float32) ** level_of(streams_of[7], (D,), ((0, 4),), -0.2, 0.2)), 0.3, 3.0)
    return {"tokens": tokens, "gain_in": gain_in, "routes": routes, "gates": gates, "w_gate": w_gate, "w_up": w_up, "w_down": w_down, "gain_out": gain_out}


EPS = 1e-06

def reference(tokens, gain_in, routes, gates, w_gate, w_up, w_down, gain_out):
    values = tokens.astype(jnp.float32)
    normed = (values * lax.rsqrt(lax.optimization_barrier(jnp.mean(values * values, axis=-1, keepdims=True)) + EPS) * gain_in).astype(jnp.bfloat16)
    most = N_EP * N_TP * CAP
    blocks = FF // FF_DEV

    def one_expert(total, items):
        expert, gate_w, up_w, down_w = items
        hit = routes == expert
        chosen = jnp.any(hit, axis=1)
        index = jnp.nonzero(chosen, size=most, fill_value=0)[0].astype(jnp.int32)
        count = jnp.sum(chosen.astype(jnp.int32))
        live = (jnp.arange(most, dtype=jnp.int32) < count).astype(jnp.float32)
        rows = normed[index]
        gate = jnp.dot(rows, gate_w, preferred_element_type=jnp.float32)
        up = jnp.dot(rows, up_w, preferred_element_type=jnp.float32)
        hidden = (jax.nn.silu(gate) * up).astype(jnp.bfloat16)
        parts = jnp.einsum('rbf,bfd->brd', hidden.reshape(most, blocks, FF_DEV).astype(jnp.float32), down_w.reshape(blocks, FF_DEV, D).astype(jnp.float32))
        rounded = lax.optimization_barrier(parts.astype(jnp.bfloat16))
        summed = lax.optimization_barrier(jnp.sum(rounded.astype(jnp.float32), axis=0))
        result = lax.optimization_barrier(summed.astype(jnp.bfloat16)).astype(jnp.float32)
        weight = lax.optimization_barrier(jnp.sum(jnp.where(hit, gates, jnp.float32(0.0)), axis=1))[index] * live
        total = total.at[index].add(weight[:, None] * result)
        return (total, None)
    start = jnp.zeros((TOKENS, D), jnp.float32)
    combined, unused = lax.scan(one_expert, start, (jnp.arange(EXPERTS, dtype=jnp.int32), w_gate, w_up, w_down))
    scale = lax.rsqrt(lax.optimization_barrier(jnp.mean(combined * combined, axis=-1, keepdims=True)) + EPS)
    return (combined * scale * gain_out).astype(jnp.bfloat16)
```

```python
import functools

import jax
import jax.numpy as jnp
from jax import lax
from jax.experimental import pallas as pl
from jax.experimental.pallas import tpu as pltpu
from jax.sharding import PartitionSpec as P

EPS = 1e-06
MESH = pl.DeviceIdType.MESH
BF = jnp.bfloat16
F32 = jnp.float32


def layer_kernel(
    experts, groups, cap,
    tokens_ref, gain_ref, routes_ref, gates_ref, wg_hbm, wu_hbm, wd_hbm, gout_ref,
    out_ref,
    wg, wu, wd, piece, column, select, slots, rows, hidden, partial, terms, result, answers, comb_hi, comb_lo, squares,
    w_sem, xa_s, xa_r, zs_s, zs_r, ag_s, ag_r, rs_s, rs_r, zr_s, zr_r, sq_s, sq_r,
):
    grp, ep, tp = lax.axis_index("grp"), lax.axis_index("ep"), lax.axis_index("tp")
    z, c = ep // 2, ep % 2
    nz = experts // 2
    count, width = tokens_ref.shape
    local_tokens = groups * count
    slice_width = width // groups
    block = groups * cap
    per_chunk = 4
    chunks = experts // per_chunk
    chunk_rows = per_chunk * block
    hidden_width = wg.shape[1]

    def offsets(k):
        far = jnp.where(k == 0, 1, nz // 2 + 1 - k)
        return jnp.where(k == 1, 0, far), jnp.where(k == 1, nz // 2, nz - far)

    def expert_at(k, j):
        first, second = offsets(k)
        d = first if j < 2 else second
        return ((z + d) % nz) * 2 + (c + j % 2) % 2

    def source_at(k, j):
        first, second = offsets(k)
        d = first if j < 2 else second
        return ((z + nz - d) % nz) * 2 + (c + j % 2) % 2

    def peer(j):
        return (tp + j) % groups

    def giver(j):
        return (tp + groups - j) % groups

    barrier = pltpu.get_barrier_semaphore()
    for j in range(1, groups):
        pl.semaphore_signal(barrier, inc=1, device_id=(grp, ep, peer(j)), device_id_type=MESH)

    def greet(i, carry):
        pl.semaphore_signal(barrier, inc=1, device_id=(grp, (ep + i) % experts, tp), device_id_type=MESH)
        return carry

    lax.fori_loop(1, experts, greet, 0)

    w_copies = [
        pltpu.make_async_copy(src.at[0], dst, w_sem.at[i])
        for i, (src, dst) in enumerate(((wg_hbm, wg), (wu_hbm, wu), (wd_hbm, wd)))
    ]
    for copy in w_copies:
        copy.start()

    values = tokens_ref[...].astype(F32)
    normed = values * lax.rsqrt(jnp.mean(values * values, axis=-1, keepdims=True) + EPS) * gain_ref[...]
    normed = normed.astype(BF)
    for q in range(groups):
        piece[q] = normed[:, q * slice_width:(q + 1) * slice_width]

    at = lax.broadcasted_iota(jnp.int32, (experts, local_tokens), 0)
    k_of, j_of = at // per_chunk, at % per_chunk
    first, second = offsets(k_of)
    d_of = jnp.where(j_of < 2, first, second)
    expert = ((z + d_of) % nz) * 2 + (c + j_of % 2) % 2
    hit0 = routes_ref[0:1, :] == expert
    hit1 = routes_ref[1:2, :] == expert
    zero = jnp.zeros((), F32)
    one = jnp.ones((), F32)
    hit = jnp.where(hit0, one, zero) + jnp.where(hit1, one, zero)
    before = (
        lax.broadcasted_iota(jnp.int32, (local_tokens, local_tokens), 0)
        < lax.broadcasted_iota(jnp.int32, (local_tokens, local_tokens), 1)
    )
    before = jnp.where(before, one, zero).astype(BF)
    rank = jnp.dot(hit.astype(BF), before, preferred_element_type=F32)
    rank = jnp.where(hit > 0, rank, -one)
    gate = jnp.where(hit0, gates_ref[0:1, :], zero) + jnp.where(hit1, gates_ref[1:2, :], zero)
    slot_of = lax.broadcasted_iota(jnp.int32, (experts, block, local_tokens), 1).astype(F32)
    chosen = rank[:, None, :] == slot_of
    select[...] = jnp.where(chosen, one, zero).reshape(experts * block, local_tokens).astype(BF)

    pl.semaphore_wait(barrier, groups - 1 + experts - 1)

    def xa_copy(j, src, dst, device):
        return pltpu.make_async_remote_copy(
            src_ref=piece.at[src], dst_ref=column.at[dst], send_sem=xa_s.at[j - 1], recv_sem=xa_r.at[j - 1],
            device_id=(grp, ep, device), device_id_type=MESH)

    for j in range(1, groups):
        xa_copy(j, peer(j), tp, peer(j)).start()
    column[tp] = piece[tp]
    for j in range(1, groups):
        xa_copy(j, peer(j), giver(j), peer(j)).wait_recv()

    def zs_copy(k, j):
        pos = k * per_chunk + j
        return pltpu.make_async_remote_copy(
            src_ref=slots.at[pos], dst_ref=rows.at[tp, pos], send_sem=zs_s.at[pos], recv_sem=zs_r.at[pos],
            device_id=(grp, expert_at(k, j), tp), device_id_type=MESH)

    def each(k, action):
        for j in range(per_chunk):
            if j == 0:
                @pl.when(k != 1)
                def _():
                    action(j)
            else:
                action(j)

    features = column[...].reshape(local_tokens, slice_width)

    def dispatch(k, carry):
        picked = jnp.dot(
            select[pl.ds(pl.multiple_of(k * chunk_rows, chunk_rows), chunk_rows), :],
            features, preferred_element_type=F32)
        slots[pl.ds(k * per_chunk, per_chunk)] = picked.reshape(per_chunk, block, slice_width).astype(BF)
        each(k, lambda j: zs_copy(k, j).start())
        return carry

    lax.fori_loop(0, chunks, dispatch, 0)
    rows[tp, per_chunk] = slots[per_chunk]

    high = gate.astype(BF).astype(F32)
    low = gate - high
    comb_hi[...] = jnp.where(chosen, high[:, None, :], zero).reshape(experts * block, local_tokens).T.astype(BF)
    comb_lo[...] = jnp.where(chosen, low[:, None, :], zero).reshape(experts * block, local_tokens).T.astype(BF)

    for copy in w_copies:
        copy.wait()

    def span(k):
        return pl.ds(k * per_chunk, per_chunk)

    def ag_copy(k, j, owner):
        i = k * (groups - 1) + j - 1
        return pltpu.make_async_remote_copy(
            src_ref=rows.at[tp, span(k)], dst_ref=rows.at[owner, span(k)], send_sem=ag_s.at[i], recv_sem=ag_r.at[i],
            device_id=(grp, ep, peer(j)), device_id_type=MESH)

    def rs_copy(k, j, owner):
        i = k * (groups - 1) + j - 1
        return pltpu.make_async_remote_copy(
            src_ref=partial.at[peer(j), span(k)], dst_ref=terms.at[owner, span(k)],
            send_sem=rs_s.at[i], recv_sem=rs_r.at[i],
            device_id=(grp, ep, peer(j)), device_id_type=MESH)

    def zr_copy(k, j):
        pos = k * per_chunk + j
        return pltpu.make_async_remote_copy(
            src_ref=result.at[pos], dst_ref=answers.at[pos], send_sem=zr_s.at[pos], recv_sem=zr_r.at[pos],
            device_id=(grp, source_at(k, j), tp), device_id_type=MESH)

    def gather(k):
        each(k, lambda j: zs_copy(k, j).wait_recv())
        for j in (1, 3, 2):
            ag_copy(k, j, tp).start()

    def compute(k):
        for j in range(1, groups):
            ag_copy(k, j, giver(j)).wait_recv()
        x = jnp.concatenate(
            [rows[q, span(k)].reshape(chunk_rows, slice_width) for q in range(groups)], axis=1)
        step = 256
        for n in range(hidden_width // step):
            cols = slice(n * step, (n + 1) * step)
            g = jnp.dot(x, wg[:, cols], preferred_element_type=F32)
            u = jnp.dot(x, wu[:, cols], preferred_element_type=F32)
            hidden[:, cols] = (g * (1.0 / (1.0 + jnp.exp(-g))) * u).astype(BF)
        h = hidden[...]
        for j in (1, 3, 2, 0):
            q = peer(j)
            part = jnp.dot(
                h, wd[:, pl.ds(pl.multiple_of(q * slice_width, slice_width), slice_width)],
                preferred_element_type=F32)
            partial[q, span(k)] = part.reshape(per_chunk, block, slice_width).astype(BF)
            if j != 0:
                rs_copy(k, j, tp).start()

    def give_back(k):
        for j in range(1, groups):
            rs_copy(k, j, giver(j)).wait_recv()
        total = partial[tp, span(k)].astype(F32)
        for j in range(1, groups):
            total += terms[giver(j), span(k)].astype(F32)
        result[span(k)] = total.astype(BF)
        each(k, lambda j: zr_copy(k, j).start())

    def pipeline(s, carry):
        @pl.when(s < chunks)
        def _():
            gather(s)

        @pl.when((s >= 1) & (s <= chunks))
        def _():
            compute(s - 1)

        @pl.when(s >= 2)
        def _():
            give_back(s - 2)
        return carry

    lax.fori_loop(0, chunks + 2, pipeline, 0)
    answers[per_chunk] = result[per_chunk]

    def collect(k, carry):
        each(k, lambda j: zr_copy(k, j).wait_recv())
        return carry

    lax.fori_loop(0, chunks, collect, 0)
    outs = answers[...].reshape(experts * block, slice_width)
    combined = jnp.dot(comb_hi[...], outs, preferred_element_type=F32)
    combined += jnp.dot(comb_lo[...], outs, preferred_element_type=F32)

    own = jnp.sum(combined * combined, axis=1, keepdims=True)
    squares[tp] = jnp.broadcast_to(own, (local_tokens, 128)).T[:8]

    def sq_copy(j, owner):
        return pltpu.make_async_remote_copy(
            src_ref=squares.at[tp], dst_ref=squares.at[owner], send_sem=sq_s.at[j - 1], recv_sem=sq_r.at[j - 1],
            device_id=(grp, ep, peer(j)), device_id_type=MESH)

    for j in range(1, groups):
        sq_copy(j, tp).start()
    for j in range(1, groups):
        sq_copy(j, giver(j)).wait_recv()
    total = squares[0] + squares[1] + squares[2] + squares[3]
    scale = lax.rsqrt(total / width + EPS)
    scale = jnp.concatenate([scale] * 16, axis=0).T[:, :1]
    out_ref[...] = (combined * scale * gout_ref[...]).astype(BF)

    def drain(k, carry):
        each(k, lambda j: zs_copy(k, j).wait_send())
        each(k, lambda j: zr_copy(k, j).wait_send())
        for j in range(1, groups):
            ag_copy(k, j, tp).wait_send()
            rs_copy(k, j, tp).wait_send()
        return carry

    lax.fori_loop(0, chunks, drain, 0)
    for j in range(1, groups):
        xa_copy(j, peer(j), tp, peer(j)).wait_send()
        sq_copy(j, tp).wait_send()


def local(tokens, gain_in, routes, gates, w_gate, w_up, w_down, gain_out):
    count, width = tokens.shape
    choose = routes.shape[1]
    experts = lax.axis_size("ep")
    groups = lax.axis_size("tp")
    cap = (3 * count * choose + 2 * experts - 1) // (2 * experts)
    hidden_width = w_gate.shape[2]
    slice_width = width // groups
    block = groups * cap
    tokens_here = groups * count
    chunks = experts // 4
    vmem = pl.BlockSpec(memory_space=pltpu.VMEM)
    hbm = pl.BlockSpec(memory_space=pl.ANY)
    dma = pltpu.SemaphoreType.DMA
    return pl.pallas_call(
        functools.partial(layer_kernel, experts, groups, cap),
        out_shape=jax.ShapeDtypeStruct((tokens_here, slice_width), BF),
        in_specs=[vmem, vmem, vmem, vmem, hbm, hbm, hbm, vmem],
        out_specs=vmem,
        scratch_shapes=[
            pltpu.VMEM((width, hidden_width), BF),
            pltpu.VMEM((width, hidden_width), BF),
            pltpu.VMEM((hidden_width, width), BF),
            pltpu.VMEM((groups, count, slice_width), BF),
            pltpu.VMEM((groups, count, slice_width), BF),
            pltpu.VMEM((experts * block, tokens_here), BF),
            pltpu.VMEM((experts, block, slice_width), BF),
            pltpu.VMEM((groups, experts, block, slice_width), BF),
            pltpu.VMEM((4 * block, hidden_width), BF),
            pltpu.VMEM((groups, experts, block, slice_width), BF),
            pltpu.VMEM((groups, experts, block, slice_width), BF),
            pltpu.VMEM((experts, block, slice_width), BF),
            pltpu.VMEM((experts, block, slice_width), BF),
            pltpu.VMEM((tokens_here, experts * block), BF),
            pltpu.VMEM((tokens_here, experts * block), BF),
            pltpu.VMEM((groups, 8, tokens_here), F32),
            dma((3,)),
            dma((groups - 1,)), dma((groups - 1,)),
            dma((experts,)), dma((experts,)),
            dma((chunks * (groups - 1),)), dma((chunks * (groups - 1),)),
            dma((chunks * (groups - 1),)), dma((chunks * (groups - 1),)),
            dma((experts,)), dma((experts,)),
            dma((groups - 1,)), dma((groups - 1,)),
        ],
        compiler_params=pltpu.CompilerParams(
            collective_id=0, has_side_effects=True, vmem_limit_bytes=56 * 1024 * 1024),
        name="routed_experts",
    )(tokens, gain_in.reshape(1, width), routes.T, gates.T, w_gate, w_up, w_down, gain_out.reshape(1, slice_width))


def solution(mesh):
    in_specs = (
        P(("grp", "ep", "tp"), None),
        P(),
        P(("grp", "ep"), None),
        P(("grp", "ep"), None),
        P("ep", None, "tp"),
        P("ep", None, "tp"),
        P("ep", "tp", None),
        P("tp"),
    )
    out_specs = P(("grp", "ep"), "tp")
    return jax.shard_map(local, mesh=mesh, in_specs=in_specs, out_specs=out_specs, check_vma=False)
```

```python
import functools

import jax
import jax.numpy as jnp
from jax import lax
from jax.experimental import pallas as pl
from jax.experimental.pallas import tpu as pltpu
from jax.sharding import PartitionSpec as P

EPS = 1e-06
MESH = pl.DeviceIdType.MESH
BF = jnp.bfloat16
F32 = jnp.float32
OWN = 8
EARLY = 6


def layer_kernel(
    experts, groups, cap,
    tokens_ref, gain_ref, routes_ref, gates_ref, wg_hbm, wu_hbm, wd_hbm, gout_ref,
    out_ref,
    wg, wu, wd, piece, column, select, slots, rows, hidden, partial, raw, terms, result, answers, comb_hi, comb_lo, squares,
    ready, w_sem, xa_s, xa_r, zs_s, zs_r, ag_s, ag_r, re_s, re_r, ra_s, ra_r, rs_s, rs_r, zr_s, zr_r, sq_s, sq_r,
):
    grp, ep, tp = lax.axis_index("grp"), lax.axis_index("ep"), lax.axis_index("tp")
    z, c = ep // 2, ep % 2
    nz = experts // 2
    count, width = tokens_ref.shape
    local_tokens = groups * count
    slice_width = width // groups
    block = groups * cap
    per_chunk = 2
    chunks = experts // per_chunk
    chunk_rows = per_chunk * block
    hidden_width = wg.shape[1]

    half = nz // 2

    def ahead(s):
        u = jnp.where(s > OWN, s - 1, s)
        mixed = jnp.where(u % 2 == 1, (u + 3) // 2, half + u // 2)
        return jnp.where(s == OWN, 0, jnp.where(u == 0, 1, mixed))

    def expert_at(s, j):
        return ((z + nz - ahead(s)) % nz) * 2 + (c + j) % 2

    def source_at(s, j):
        return ((z + ahead(s)) % nz) * 2 + (c + j) % 2

    rank_here = (ep + experts - 1) % experts

    def at_rank(r):
        return (r + 1) % experts

    def peer(j):
        return (tp + j) % groups

    def giver(j):
        return (tp + groups - j) % groups

    barrier = pltpu.get_barrier_semaphore()

    def signal(sem, device):
        pl.semaphore_signal(sem, inc=1, device_id=device, device_id_type=MESH)

    for j in range(1, groups):
        signal(barrier, (grp, ep, peer(j)))

    def greet(r, carry):
        signal(barrier, (grp, at_rank(r), tp))
        return carry

    lax.fori_loop(rank_here + 1, experts, greet, 0)

    w_copies = [
        pltpu.make_async_copy(src.at[0], dst, w_sem.at[i])
        for i, (src, dst) in enumerate(((wg_hbm, wg), (wu_hbm, wu), (wd_hbm, wd)))
    ]
    for copy in w_copies:
        copy.start()

    values = tokens_ref[...].astype(F32)
    normed = values * lax.rsqrt(jnp.mean(values * values, axis=-1, keepdims=True) + EPS) * gain_ref[...]
    normed = normed.astype(BF)
    for q in range(groups):
        piece[q] = normed[:, q * slice_width:(q + 1) * slice_width]

    at = lax.broadcasted_iota(jnp.int32, (experts, local_tokens), 0)
    expert = expert_at(at // per_chunk, at % per_chunk)
    hit0 = routes_ref[0:1, :] == expert
    hit1 = routes_ref[1:2, :] == expert
    zero = jnp.zeros((), F32)
    one = jnp.ones((), F32)
    hit = jnp.where(hit0, one, zero) + jnp.where(hit1, one, zero)
    before = (
        lax.broadcasted_iota(jnp.int32, (local_tokens, local_tokens), 0)
        < lax.broadcasted_iota(jnp.int32, (local_tokens, local_tokens), 1)
    )
    before = jnp.where(before, one, zero).astype(BF)
    rank = jnp.dot(hit.astype(BF), before, preferred_element_type=F32)
    rank = jnp.where(hit > 0, rank, -one)
    gate = jnp.where(hit0, gates_ref[0:1, :], zero) + jnp.where(hit1, gates_ref[1:2, :], zero)
    slot_of = lax.broadcasted_iota(jnp.int32, (experts, block, local_tokens), 1).astype(F32)
    chosen = rank[:, None, :] == slot_of
    select[...] = jnp.where(chosen, one, zero).reshape(experts * block, local_tokens).astype(BF)

    with jax.named_scope("entry"):
        pl.semaphore_wait(barrier, groups - 1 + rank_here)

    def answer(r, carry):
        signal(ready.at[ep], (grp, at_rank(r), tp))
        return carry

    lax.fori_loop(0, rank_here, answer, 0)

    def xa_copy(j, src, dst, device):
        return pltpu.make_async_remote_copy(
            src_ref=piece.at[src], dst_ref=column.at[dst], send_sem=xa_s.at[j - 1], recv_sem=xa_r.at[j - 1],
            device_id=(grp, ep, device), device_id_type=MESH)

    for j in range(1, groups):
        xa_copy(j, peer(j), tp, peer(j)).start()
    column[tp] = piece[tp]
    with jax.named_scope("slices"):
        for j in range(1, groups):
            xa_copy(j, peer(j), giver(j), peer(j)).wait_recv()

    def zs_copy(s, j):
        pos = s * per_chunk + j
        return pltpu.make_async_remote_copy(
            src_ref=slots.at[pos], dst_ref=rows.at[tp, pos], send_sem=zs_s.at[pos], recv_sem=zs_r.at[pos],
            device_id=(grp, expert_at(s, j), tp), device_id_type=MESH)

    def each(s, action):
        @pl.when(s != OWN)
        def _():
            action(0)

        action(1)

    def send(s, now):
        k = ahead(s)

        def one(j):
            other = expert_at(s, j)
            higher = (other + experts - 1) % experts > rank_here
            back = jnp.where((k == 0) & (other != 0), 0, (7 * (nz - k)) // 16)
            shift = jnp.where(higher, back, 0 - (7 * k) // 16)
            leave_at = jnp.minimum(jnp.maximum(s - EARLY + shift, 0), chunks - 1)

            @pl.when((leave_at == now) & higher)
            def _():
                pl.semaphore_wait(ready.at[other], 1)

            @pl.when(leave_at == now)
            def _():
                zs_copy(s, j).start()

        each(s, one)

    features = column[...].reshape(local_tokens, slice_width)

    def dispatch(k, carry):
        picked = jnp.dot(
            select[pl.ds(pl.multiple_of(k * chunk_rows, chunk_rows), chunk_rows), :],
            features, preferred_element_type=F32)
        slots[pl.ds(k * per_chunk, per_chunk)] = picked.reshape(per_chunk, block, slice_width).astype(BF)

        send(k, 0)
        return carry

    with jax.named_scope("dispatch"):
        lax.fori_loop(0, chunks, dispatch, 0)
    rows[tp, OWN * per_chunk] = slots[OWN * per_chunk]

    high = gate.astype(BF).astype(F32)
    low = gate - high
    comb_hi[...] = jnp.where(chosen, high[:, None, :], zero).reshape(experts * block, local_tokens).T.astype(BF)
    comb_lo[...] = jnp.where(chosen, low[:, None, :], zero).reshape(experts * block, local_tokens).T.astype(BF)

    with jax.named_scope("weights"):
        for copy in w_copies:
            copy.wait()

    def span(k):
        return pl.ds(k * per_chunk, per_chunk)

    def neighbour(way):
        return peer(1) if way == 0 else peer(groups - 1)

    def move(src, dst, send, recv, k, way):
        i = k * 2 + way
        return pltpu.make_async_remote_copy(
            src_ref=src, dst_ref=dst, send_sem=send.at[i], recv_sem=recv.at[i],
            device_id=(grp, ep, neighbour(way)), device_id_type=MESH)

    def ag_copy(k, way, owner):
        return move(rows.at[tp, span(k)], rows.at[owner, span(k)], ag_s, ag_r, k, way)

    def re_copy(k, way, src, dst):
        pos = k * per_chunk + way
        return move(rows.at[src, pos], rows.at[dst, pos], re_s, re_r, k, way)

    def ra_copy(k, way):
        pos = k * per_chunk + way
        return move(partial.at[peer(2), pos], raw.at[pos], ra_s, ra_r, k, way)

    def rs_copy(k, way):
        return move(partial.at[neighbour(way), span(k)], terms.at[way, span(k)], rs_s, rs_r, k, way)

    def zr_copy(k, j):
        pos = k * per_chunk + j
        return pltpu.make_async_remote_copy(
            src_ref=result.at[pos], dst_ref=answers.at[pos], send_sem=zr_s.at[pos], recv_sem=zr_r.at[pos],
            device_id=(grp, source_at(k, j), tp), device_id_type=MESH)

    def gather(k):
        with jax.named_scope("rows_wait"):
            each(k, lambda j: zs_copy(k, j).wait_recv())
        for way in range(2):
            ag_copy(k, way, tp).start()

    def relay(k):
        for way in range(2):
            with jax.named_scope("gather_wait"):
                ag_copy(k, way, neighbour(1 - way)).wait_recv()
            re_copy(k, way, neighbour(1 - way), neighbour(1 - way)).start()

    def compute(k):
        with jax.named_scope("relay_wait"):
            for way in range(2):
                re_copy(k, way, neighbour(1 - way), peer(2)).wait_recv()
        x = jnp.concatenate(
            [rows[q, span(k)].reshape(chunk_rows, slice_width) for q in range(groups)], axis=1)
        step = 256
        for n in range(hidden_width // step):
            cols = slice(n * step, (n + 1) * step)
            g = jnp.dot(x, wg[:, cols], preferred_element_type=F32)
            u = jnp.dot(x, wu[:, cols], preferred_element_type=F32)
            hidden[:, cols] = (g * (1.0 / (1.0 + jnp.exp(-g))) * u).astype(BF)
        h = hidden[...]
        for j in (2, 1, 3, 0):
            q = peer(j)
            part = jnp.dot(
                h, wd[:, pl.ds(pl.multiple_of(q * slice_width, slice_width), slice_width)],
                preferred_element_type=F32)
            partial[q, span(k)] = part.reshape(per_chunk, block, slice_width).astype(BF)
            if j == 1:
                for way in range(2):
                    ra_copy(k, way).start()

    def forward(k):
        for way in range(2):
            with jax.named_scope("raw_wait"):
                ra_copy(k, way).wait_recv()
            pos = k * per_chunk + way
            both = partial[neighbour(way), pos].astype(F32) + raw[pos].astype(F32)
            partial[neighbour(way), pos] = both.astype(BF)
        for way in range(2):
            rs_copy(k, way).start()

    def give_back(k):
        with jax.named_scope("terms_wait"):
            for way in range(2):
                rs_copy(k, way).wait_recv()
        total = partial[tp, span(k)].astype(F32)
        for way in range(2):
            total += terms[way, span(k)].astype(F32)
        result[span(k)] = total.astype(BF)
        each(k, lambda j: zr_copy(k, j).start())

    def pipeline(s, carry):
        def send_due(later, inner):
            send(later, s)
            return inner

        @pl.when((s > 0) & (s < chunks))
        def _():
            with jax.named_scope("ready_wait"):
                lax.fori_loop(0, chunks, send_due, 0)

        for lag, stage in ((6, forward), (8, give_back), (2, relay), (4, compute), (0, gather)):
            @pl.when((s >= lag) & (s < chunks + lag))
            def _(lag=lag, stage=stage):
                stage(s - lag)
        return carry

    lax.fori_loop(0, chunks + 8, pipeline, 0)
    answers[OWN * per_chunk] = result[OWN * per_chunk]

    def collect(k, carry):
        each(k, lambda j: zr_copy(k, j).wait_recv())
        return carry

    with jax.named_scope("answers_wait"):
        lax.fori_loop(0, chunks, collect, 0)
    outs = answers[...].reshape(experts * block, slice_width)
    combined = jnp.dot(comb_hi[...], outs, preferred_element_type=F32)
    combined += jnp.dot(comb_lo[...], outs, preferred_element_type=F32)

    own = jnp.sum(combined * combined, axis=1, keepdims=True)
    squares[tp] = jnp.broadcast_to(own, (local_tokens, 128)).T[:8]

    def sq_copy(j, owner):
        return pltpu.make_async_remote_copy(
            src_ref=squares.at[tp], dst_ref=squares.at[owner], send_sem=sq_s.at[j - 1], recv_sem=sq_r.at[j - 1],
            device_id=(grp, ep, peer(j)), device_id_type=MESH)

    for j in range(1, groups):
        sq_copy(j, tp).start()
    with jax.named_scope("squares_wait"):
        for j in range(1, groups):
            sq_copy(j, giver(j)).wait_recv()
    total = squares[0] + squares[1] + squares[2] + squares[3]
    scale = lax.rsqrt(total / width + EPS)
    scale = jnp.concatenate([scale] * 16, axis=0).T[:, :1]
    out_ref[...] = (combined * scale * gout_ref[...]).astype(BF)

    def drain(k, carry):
        each(k, lambda j: zs_copy(k, j).wait_send())
        each(k, lambda j: zr_copy(k, j).wait_send())
        for way in range(2):
            ag_copy(k, way, tp).wait_send()
            re_copy(k, way, tp, tp).wait_send()
            ra_copy(k, way).wait_send()
            rs_copy(k, way).wait_send()
        return carry

    with jax.named_scope("drain"):
        lax.fori_loop(0, chunks, drain, 0)
    for j in range(1, groups):
        xa_copy(j, peer(j), tp, peer(j)).wait_send()
        sq_copy(j, tp).wait_send()


def local(tokens, gain_in, routes, gates, w_gate, w_up, w_down, gain_out):
    count, width = tokens.shape
    choose = routes.shape[1]
    experts = lax.axis_size("ep")
    groups = lax.axis_size("tp")
    cap = (3 * count * choose + 2 * experts - 1) // (2 * experts)
    hidden_width = w_gate.shape[2]
    slice_width = width // groups
    block = groups * cap
    tokens_here = groups * count
    chunks = experts // 2
    vmem = pl.BlockSpec(memory_space=pltpu.VMEM)
    hbm = pl.BlockSpec(memory_space=pl.ANY)
    dma = pltpu.SemaphoreType.DMA
    return pl.pallas_call(
        functools.partial(layer_kernel, experts, groups, cap),
        out_shape=jax.ShapeDtypeStruct((tokens_here, slice_width), BF),
        in_specs=[vmem, vmem, vmem, vmem, hbm, hbm, hbm, vmem],
        out_specs=vmem,
        scratch_shapes=[
            pltpu.VMEM((width, hidden_width), BF),
            pltpu.VMEM((width, hidden_width), BF),
            pltpu.VMEM((hidden_width, width), BF),
            pltpu.VMEM((groups, count, slice_width), BF),
            pltpu.VMEM((groups, count, slice_width), BF),
            pltpu.VMEM((experts * block, tokens_here), BF),
            pltpu.VMEM((experts, block, slice_width), BF),
            pltpu.VMEM((groups, experts, block, slice_width), BF),
            pltpu.VMEM((2 * block, hidden_width), BF),
            pltpu.VMEM((groups, experts, block, slice_width), BF),
            pltpu.VMEM((experts, block, slice_width), BF),
            pltpu.VMEM((2, experts, block, slice_width), BF),
            pltpu.VMEM((experts, block, slice_width), BF),
            pltpu.VMEM((experts, block, slice_width), BF),
            pltpu.VMEM((tokens_here, experts * block), BF),
            pltpu.VMEM((tokens_here, experts * block), BF),
            pltpu.VMEM((groups, 8, tokens_here), F32),
            pltpu.SemaphoreType.REGULAR((experts,)),
            dma((3,)),
            dma((groups - 1,)), dma((groups - 1,)),
            dma((experts,)), dma((experts,)),
            *[dma((chunks * 2,)) for _ in range(8)],
            dma((experts,)), dma((experts,)),
            dma((groups - 1,)), dma((groups - 1,)),
        ],
        compiler_params=pltpu.CompilerParams(
            collective_id=0, has_side_effects=True, vmem_limit_bytes=56 * 1024 * 1024),
        name="routed_experts",
    )(tokens, gain_in.reshape(1, width), routes.T, gates.T, w_gate, w_up, w_down, gain_out.reshape(1, slice_width))


def solution(mesh):
    in_specs = (
        P(("grp", "ep", "tp"), None),
        P(),
        P(("grp", "ep"), None),
        P(("grp", "ep"), None),
        P("ep", None, "tp"),
        P("ep", None, "tp"),
        P("ep", "tp", None),
        P("tp"),
    )
    out_specs = P(("grp", "ep"), "tp")
    return jax.shard_map(local, mesh=mesh, in_specs=in_specs, out_specs=out_specs, check_vma=False)
```

```python
import functools

import jax
import jax.numpy as jnp
from jax import lax
from jax.experimental import pallas as pl
from jax.experimental.pallas import tpu as pltpu
from jax.sharding import PartitionSpec as P

EPS = 1e-06
MESH = pl.DeviceIdType.MESH
BF = jnp.bfloat16
F32 = jnp.float32
OWN = 6
NEAR = 4
EARLY = 8


def layer_kernel(
    experts, groups, cap,
    tokens_ref, gain_ref, routes_ref, gates_ref, wg_hbm, wu_hbm, wd_hbm, gout_ref,
    out_ref,
    wg, wu, wd, piece, column, select, slots, rows, hidden, partial, raw, terms, result, answers, comb_hi, comb_lo, squares,
    ready, w_sem, xa_s, xa_r, zs_s, zs_r, ag_s, ag_r, re_s, re_r, ra_s, ra_r, rs_s, rs_r, zr_s, zr_r, sq_s, sq_r,
):
    grp, ep, tp = lax.axis_index("grp"), lax.axis_index("ep"), lax.axis_index("tp")
    z, c = ep // 2, ep % 2
    nz = experts // 2
    count, width = tokens_ref.shape
    local_tokens = groups * count
    slice_width = width // groups
    block = groups * cap
    per_chunk = 2
    chunks = experts // per_chunk
    chunk_rows = per_chunk * block
    hidden_width = wg.shape[1]

    half = nz // 2

    def pick(condition, yes, no):
        if isinstance(condition, (bool, int)):
            return yes if condition else no
        return jnp.where(condition, yes, no)

    def ahead(s):
        u = pick(s > OWN, s - 1, s)
        v = u - NEAR
        mixed = pick(v % 2 == 0, half + 1 + v // 2, NEAR + (v + 1) // 2)
        later = pick(v < 2 * (half - NEAR), mixed, u + 1)
        return pick(s == OWN, 0, pick(u < NEAR, u + 1, later))

    def expert_at(s, j):
        return ((z + nz - ahead(s)) % nz) * 2 + (c + j) % 2

    def source_at(s, j):
        return ((z + ahead(s)) % nz) * 2 + (c + j) % 2

    rank_here = (ep + experts - 1) % experts

    def at_rank(r):
        return (r + 1) % experts

    def peer(j):
        return (tp + j) % groups

    def giver(j):
        return (tp + groups - j) % groups

    barrier = pltpu.get_barrier_semaphore()

    def signal(sem, device):
        pl.semaphore_signal(sem, inc=1, device_id=device, device_id_type=MESH)

    for j in range(1, groups):
        signal(barrier, (grp, ep, peer(j)))

    def greet(r, carry):
        signal(barrier, (grp, at_rank(r), tp))
        return carry

    lax.fori_loop(rank_here + 1, experts, greet, 0)

    w_copies = [
        pltpu.make_async_copy(src.at[0], dst, w_sem.at[i])
        for i, (src, dst) in enumerate(((wg_hbm, wg), (wu_hbm, wu), (wd_hbm, wd)))
    ]
    for copy in w_copies:
        copy.start()

    values = tokens_ref[...].astype(F32)
    normed = values * lax.rsqrt(jnp.mean(values * values, axis=-1, keepdims=True) + EPS) * gain_ref[...]
    normed = normed.astype(BF)
    for q in range(groups):
        piece[q] = normed[:, q * slice_width:(q + 1) * slice_width]

    at = lax.broadcasted_iota(jnp.int32, (experts, local_tokens), 0)
    expert = expert_at(at // per_chunk, at % per_chunk)
    hit0 = routes_ref[0:1, :] == expert
    hit1 = routes_ref[1:2, :] == expert
    zero = jnp.zeros((), F32)
    one = jnp.ones((), F32)
    hit = jnp.where(hit0, one, zero) + jnp.where(hit1, one, zero)
    before = (
        lax.broadcasted_iota(jnp.int32, (local_tokens, local_tokens), 0)
        < lax.broadcasted_iota(jnp.int32, (local_tokens, local_tokens), 1)
    )
    before = jnp.where(before, one, zero).astype(BF)
    rank = jnp.dot(hit.astype(BF), before, preferred_element_type=F32)
    rank = jnp.where(hit > 0, rank, -one)
    gate = jnp.where(hit0, gates_ref[0:1, :], zero) + jnp.where(hit1, gates_ref[1:2, :], zero)
    slot_of = lax.broadcasted_iota(jnp.int32, (experts, block, local_tokens), 1).astype(F32)
    chosen = rank[:, None, :] == slot_of
    select[...] = jnp.where(chosen, one, zero).reshape(experts * block, local_tokens).astype(BF)

    with jax.named_scope("entry"):
        pl.semaphore_wait(barrier, groups - 1 + rank_here)

    def answer(r, carry):
        signal(ready.at[ep], (grp, at_rank(r), tp))
        return carry

    lax.fori_loop(0, rank_here, answer, 0)

    def xa_copy(j, src, dst, device):
        return pltpu.make_async_remote_copy(
            src_ref=piece.at[src], dst_ref=column.at[dst], send_sem=xa_s.at[j - 1], recv_sem=xa_r.at[j - 1],
            device_id=(grp, ep, device), device_id_type=MESH)

    for j in range(1, groups):
        xa_copy(j, peer(j), tp, peer(j)).start()
    column[tp] = piece[tp]
    with jax.named_scope("slices"):
        for j in range(1, groups):
            xa_copy(j, peer(j), giver(j), peer(j)).wait_recv()

    def zs_copy(s, j):
        pos = s * per_chunk + j
        return pltpu.make_async_remote_copy(
            src_ref=slots.at[pos], dst_ref=rows.at[tp, pos], send_sem=zs_s.at[0], recv_sem=zs_r.at[s],
            device_id=(grp, expert_at(s, j), tp), device_id_type=MESH)

    def each(s, action):
        if isinstance(s, int):
            if s != OWN:
                action(0)
        else:
            @pl.when(s != OWN)
            def _():
                action(0)

        action(1)

    def send(s, now):
        k = ahead(s)

        def one(j):
            other = expert_at(s, j)
            higher = (ep != 0) & ((z < k) | (other == 0) | ((k == 0) & (c == 0)))
            behind = (7 * (nz - k)) // 16
            behind = pick(k == 0, jnp.where(other == 0, behind, 0), behind)
            after = jnp.maximum(jnp.maximum(s - EARLY, -2) + behind, 1)
            before = s - EARLY - (7 * k) // 16
            before = max(before, 0) if isinstance(s, int) else jnp.maximum(before, 0)
            leave_at = jnp.minimum(jnp.where(higher, after, before), chunks - 1)

            @pl.when(leave_at == now)
            def _():
                @pl.when(higher)
                def _():
                    pl.semaphore_wait(ready.at[other], 1)

                zs_copy(s, j).start()

        each(s, one)

    features = column[...].reshape(local_tokens, slice_width)

    def dispatch(k, carry):
        picked = jnp.dot(
            select[pl.ds(pl.multiple_of(k * chunk_rows, chunk_rows), chunk_rows), :],
            features, preferred_element_type=F32)
        slots[pl.ds(k * per_chunk, per_chunk)] = picked.reshape(per_chunk, block, slice_width).astype(BF)

        send(k, 0)
        return carry

    with jax.named_scope("dispatch"):
        lax.fori_loop(0, chunks, dispatch, 0)
    rows[tp, OWN * per_chunk] = slots[OWN * per_chunk]

    high = gate.astype(BF).astype(F32)
    low = gate - high
    comb_hi[...] = jnp.where(chosen, high[:, None, :], zero).reshape(experts * block, local_tokens).T.astype(BF)
    comb_lo[...] = jnp.where(chosen, low[:, None, :], zero).reshape(experts * block, local_tokens).T.astype(BF)

    with jax.named_scope("weights"):
        for copy in w_copies:
            copy.wait()

    def settle(ref, sem):
        pltpu.make_async_copy(ref, ref, sem).wait()

    def span(k):
        return pl.ds(k * per_chunk, per_chunk)

    def neighbour(way):
        return peer(1) if way == 0 else peer(groups - 1)

    def move(src, dst, send, recv, k, way):
        return pltpu.make_async_remote_copy(
            src_ref=src, dst_ref=dst, send_sem=send.at[0], recv_sem=recv.at[k],
            device_id=(grp, ep, neighbour(way)), device_id_type=MESH)

    def ag_copy(k, way, owner):
        return move(rows.at[tp, span(k)], rows.at[owner, span(k)], ag_s, ag_r, k, way)

    def re_copy(k, way, src, dst):
        pos = k * per_chunk + way
        return move(rows.at[src, pos], rows.at[dst, pos], re_s, re_r, k, way)

    def ra_copy(k, way):
        pos = k * per_chunk + way
        return move(partial.at[peer(2), pos], raw.at[pos], ra_s, ra_r, k, way)

    def rs_copy(k, way):
        return move(partial.at[neighbour(way), span(k)], terms.at[way, span(k)], rs_s, rs_r, k, way)

    def zr_copy(k, j):
        pos = k * per_chunk + j
        return pltpu.make_async_remote_copy(
            src_ref=result.at[pos], dst_ref=answers.at[pos], send_sem=zr_s.at[0], recv_sem=zr_r.at[0],
            device_id=(grp, source_at(k, j), tp), device_id_type=MESH)

    def gather(k):
        with jax.named_scope("rows_wait"):
            @pl.when(k == OWN)
            def _():
                settle(rows.at[tp, k * per_chunk + 1], zs_r.at[k])

            @pl.when(k != OWN)
            def _():
                settle(rows.at[tp, span(k)], zs_r.at[k])

        for way in range(2):
            ag_copy(k, way, tp).start()

    def relay(k):
        with jax.named_scope("gather_wait"):
            settle(rows.at[:2, span(k)], ag_r.at[k])
        for way in range(2):
            re_copy(k, way, neighbour(1 - way), neighbour(1 - way)).start()

    def compute(k):
        with jax.named_scope("relay_wait"):
            settle(rows.at[peer(2), span(k)], re_r.at[k])
        x = jnp.concatenate(
            [rows[q, span(k)].reshape(chunk_rows, slice_width) for q in range(groups)], axis=1)
        step = 256
        for n in range(hidden_width // step):
            cols = slice(n * step, (n + 1) * step)
            g = jnp.dot(x, wg[:, cols], preferred_element_type=F32)
            u = jnp.dot(x, wu[:, cols], preferred_element_type=F32)
            hidden[:, cols] = (g * (1.0 / (1.0 + jnp.exp(-g))) * u).astype(BF)
        h = hidden[...]
        for j in (2, 1, 3, 0):
            q = peer(j)
            part = jnp.dot(
                h, wd[:, pl.ds(pl.multiple_of(q * slice_width, slice_width), slice_width)],
                preferred_element_type=F32)
            partial[q, span(k)] = part.reshape(per_chunk, block, slice_width).astype(BF)
            if j == 1:
                for way in range(2):
                    ra_copy(k, way).start()

    def forward(k):
        with jax.named_scope("raw_wait"):
            settle(raw.at[span(k)], ra_r.at[k])
        for way in range(2):
            pos = k * per_chunk + way
            both = partial[neighbour(way), pos].astype(F32) + raw[pos].astype(F32)
            partial[neighbour(way), pos] = both.astype(BF)
        for way in range(2):
            rs_copy(k, way).start()

    def give_back(k):
        with jax.named_scope("terms_wait"):
            settle(terms.at[:, span(k)], rs_r.at[k])
        total = partial[tp, span(k)].astype(F32)
        for way in range(2):
            total += terms[way, span(k)].astype(F32)
        result[span(k)] = total.astype(BF)
        each(k, lambda j: zr_copy(k, j).start())

    def pipeline(s, carry):
        @pl.when((s > 0) & (s < chunks))
        def _():
            with jax.named_scope("ready_wait"):
                for later in range(chunks):
                    send(later, s)

        for lag, stage in ((6, forward), (8, give_back), (2, relay), (4, compute), (0, gather)):
            @pl.when((s >= lag) & (s < chunks + lag))
            def _(lag=lag, stage=stage):
                stage(s - lag)
        return carry

    lax.fori_loop(0, chunks + 8, pipeline, 0)
    answers[OWN * per_chunk] = result[OWN * per_chunk]

    with jax.named_scope("answers_wait"):
        settle(answers.at[:experts - 1], zr_r.at[0])
    outs = answers[...].reshape(experts * block, slice_width)
    combined = jnp.dot(comb_hi[...], outs, preferred_element_type=F32)
    combined += jnp.dot(comb_lo[...], outs, preferred_element_type=F32)

    own = jnp.sum(combined * combined, axis=1, keepdims=True)
    squares[tp] = jnp.broadcast_to(own, (local_tokens, 128)).T[:8]

    def sq_copy(j, owner):
        return pltpu.make_async_remote_copy(
            src_ref=squares.at[tp], dst_ref=squares.at[owner], send_sem=sq_s.at[j - 1], recv_sem=sq_r.at[j - 1],
            device_id=(grp, ep, peer(j)), device_id_type=MESH)

    for j in range(1, groups):
        sq_copy(j, tp).start()
    with jax.named_scope("squares_wait"):
        for j in range(1, groups):
            sq_copy(j, giver(j)).wait_recv()
    total = squares[0] + squares[1] + squares[2] + squares[3]
    scale = lax.rsqrt(total / width + EPS)
    scale = jnp.concatenate([scale] * 16, axis=0).T[:, :1]
    out_ref[...] = (combined * scale * gout_ref[...]).astype(BF)

    with jax.named_scope("drain"):
        settle(slots.at[:experts - 1], zs_s.at[0])
        settle(slots.at[:experts - 1], zr_s.at[0])
        settle(rows.at[:2], ag_s.at[0])
        settle(slots, re_s.at[0])
        settle(slots, ra_s.at[0])
        settle(terms, rs_s.at[0])
    for j in range(1, groups):
        xa_copy(j, peer(j), tp, peer(j)).wait_send()
        sq_copy(j, tp).wait_send()


def local(tokens, gain_in, routes, gates, w_gate, w_up, w_down, gain_out):
    count, width = tokens.shape
    choose = routes.shape[1]
    experts = lax.axis_size("ep")
    groups = lax.axis_size("tp")
    cap = (3 * count * choose + 2 * experts - 1) // (2 * experts)
    hidden_width = w_gate.shape[2]
    slice_width = width // groups
    block = groups * cap
    tokens_here = groups * count
    chunks = experts // 2
    vmem = pl.BlockSpec(memory_space=pltpu.VMEM)
    hbm = pl.BlockSpec(memory_space=pl.ANY)
    dma = pltpu.SemaphoreType.DMA
    return pl.pallas_call(
        functools.partial(layer_kernel, experts, groups, cap),
        out_shape=jax.ShapeDtypeStruct((tokens_here, slice_width), BF),
        in_specs=[vmem, vmem, vmem, vmem, hbm, hbm, hbm, vmem],
        out_specs=vmem,
        scratch_shapes=[
            pltpu.VMEM((width, hidden_width), BF),
            pltpu.VMEM((width, hidden_width), BF),
            pltpu.VMEM((hidden_width, width), BF),
            pltpu.VMEM((groups, count, slice_width), BF),
            pltpu.VMEM((groups, count, slice_width), BF),
            pltpu.VMEM((experts * block, tokens_here), BF),
            pltpu.VMEM((experts, block, slice_width), BF),
            pltpu.VMEM((groups, experts, block, slice_width), BF),
            pltpu.VMEM((2 * block, hidden_width), BF),
            pltpu.VMEM((groups, experts, block, slice_width), BF),
            pltpu.VMEM((experts, block, slice_width), BF),
            pltpu.VMEM((2, experts, block, slice_width), BF),
            pltpu.VMEM((experts, block, slice_width), BF),
            pltpu.VMEM((experts, block, slice_width), BF),
            pltpu.VMEM((tokens_here, experts * block), BF),
            pltpu.VMEM((tokens_here, experts * block), BF),
            pltpu.VMEM((groups, 8, tokens_here), F32),
            pltpu.SemaphoreType.REGULAR((experts,)),
            dma((3,)),
            dma((groups - 1,)), dma((groups - 1,)),
            *[dma((n,)) for n in (1, chunks) * 5],
            dma((1,)), dma((1,)),
            dma((groups - 1,)), dma((groups - 1,)),
        ],
        compiler_params=pltpu.CompilerParams(
            collective_id=0, has_side_effects=True, vmem_limit_bytes=56 * 1024 * 1024),
        name="routed_experts",
    )(tokens, gain_in.reshape(1, width), routes.T, gates.T, w_gate, w_up, w_down, gain_out.reshape(1, slice_width))


def solution(mesh):
    in_specs = (
        P(("grp", "ep", "tp"), None),
        P(),
        P(("grp", "ep"), None),
        P(("grp", "ep"), None),
        P("ep", None, "tp"),
        P("ep", None, "tp"),
        P("ep", "tp", None),
        P("tp"),
    )
    out_specs = P(("grp", "ep"), "tp")
    return jax.shard_map(local, mesh=mesh, in_specs=in_specs, out_specs=out_specs, check_vma=False)
```

```python
import functools

import jax
import jax.numpy as jnp
from jax import lax
from jax.experimental import pallas as pl
from jax.experimental.pallas import tpu as pltpu
from jax.sharding import PartitionSpec as P

EPS = 1e-06
MESH = pl.DeviceIdType.MESH
BF = jnp.bfloat16
F32 = jnp.float32
NEAR = 4
EARLY = 6


def layer_kernel(
    experts, groups, cap,
    tokens_ref, gain_ref, routes_ref, gates_ref, wg_hbm, wu_hbm, wd_hbm, gout_ref,
    out_ref,
    wg, wu, wd, piece, column, select, slots, rows, hidden, partial, raw, terms, result, answers, comb_hi, comb_lo, squares,
    ready, w_sem, xa_s, xa_r, zs_s, zs_r, ag_s, ag_r, re_s, re_r, ra_s, ra_r, rs_s, rs_r, zr_s, zr_r, sq_s, sq_r,
):
    grp, ep, tp = lax.axis_index("grp"), lax.axis_index("ep"), lax.axis_index("tp")
    z, c = ep // 2, ep % 2
    nz = experts // 2
    count, width = tokens_ref.shape
    local_tokens = groups * count
    slice_width = width // groups
    block = groups * cap
    per_chunk = 2
    chunks = experts // per_chunk
    chunk_rows = per_chunk * block
    hidden_width = wg.shape[1]

    half = nz // 2
    ends = [k for i in range(1, NEAR) for k in (nz - i, i)] + [0]
    middle = [NEAR] + [k for i in range(NEAR, half - 1) for k in (nz - i, i + 1)] + [half + 1, half]
    order_low = list(range(1, NEAR + 1)) + [0, NEAR + 1] + list(range(nz - NEAR + 1, nz)) + middle[3:] + middle[1:2]
    order_low = [k for i, k in enumerate(order_low) if k not in order_low[:i]]
    order_mid = ends + middle
    order_high = ends + middle[::-1]

    def by_place(chip, low, mid, high):
        return jnp.where(chip < NEAR, low, jnp.where(chip < half, mid, high))

    here = [by_place(z, *ks) for ks in zip(order_low, order_mid, order_high)]

    def part_at(s):
        k = here[0]
        for i in range(1, nz):
            k = jnp.where(s == i, here[i], k)
        return k

    def expert_at(k, j):
        return ((z + nz - k) % nz) * 2 + (c + j) % 2

    def source_at(k, j):
        return ((z + k) % nz) * 2 + (c + j) % 2

    rank_here = (ep + experts - 1) % experts

    def at_rank(r):
        return (r + 1) % experts

    def peer(j):
        return (tp + j) % groups

    def giver(j):
        return (tp + groups - j) % groups

    barrier = pltpu.get_barrier_semaphore()

    def signal(sem, device):
        pl.semaphore_signal(sem, inc=1, device_id=device, device_id_type=MESH)

    for j in range(1, groups):
        signal(barrier, (grp, ep, peer(j)))

    def greet(r, carry):
        signal(barrier, (grp, at_rank(r), tp))
        return carry

    lax.fori_loop(rank_here + 1, experts, greet, 0)

    w_copies = [
        pltpu.make_async_copy(src.at[0], dst, w_sem.at[i])
        for i, (src, dst) in enumerate(((wg_hbm, wg), (wu_hbm, wu), (wd_hbm, wd)))
    ]
    for copy in w_copies:
        copy.start()

    values = tokens_ref[...].astype(F32)
    normed = values * lax.rsqrt(jnp.mean(values * values, axis=-1, keepdims=True) + EPS) * gain_ref[...]
    normed = normed.astype(BF)
    for q in range(groups):
        piece[q] = normed[:, q * slice_width:(q + 1) * slice_width]

    at = lax.broadcasted_iota(jnp.int32, (experts, local_tokens), 0)
    expert = expert_at(at // per_chunk, at % per_chunk)
    hit0 = routes_ref[0:1, :] == expert
    hit1 = routes_ref[1:2, :] == expert
    zero = jnp.zeros((), F32)
    one = jnp.ones((), F32)
    hit = jnp.where(hit0, one, zero) + jnp.where(hit1, one, zero)
    before = (
        lax.broadcasted_iota(jnp.int32, (local_tokens, local_tokens), 0)
        < lax.broadcasted_iota(jnp.int32, (local_tokens, local_tokens), 1)
    )
    before = jnp.where(before, one, zero).astype(BF)
    rank = jnp.dot(hit.astype(BF), before, preferred_element_type=F32)
    rank = jnp.where(hit > 0, rank, -one)
    gate = jnp.where(hit0, gates_ref[0:1, :], zero) + jnp.where(hit1, gates_ref[1:2, :], zero)
    slot_of = lax.broadcasted_iota(jnp.int32, (experts, block, local_tokens), 1).astype(F32)
    chosen = rank[:, None, :] == slot_of
    select[...] = jnp.where(chosen, one, zero).reshape(experts * block, local_tokens).astype(BF)

    with jax.named_scope("entry"):
        pl.semaphore_wait(barrier, groups - 1 + rank_here)

    def answer(r, carry):
        signal(ready.at[ep], (grp, at_rank(r), tp))
        return carry

    lax.fori_loop(0, rank_here, answer, 0)

    def xa_copy(j, src, dst, device):
        return pltpu.make_async_remote_copy(
            src_ref=piece.at[src], dst_ref=column.at[dst], send_sem=xa_s.at[j - 1], recv_sem=xa_r.at[j - 1],
            device_id=(grp, ep, device), device_id_type=MESH)

    for j in range(1, groups):
        xa_copy(j, peer(j), tp, peer(j)).start()
    column[tp] = piece[tp]
    with jax.named_scope("slices"):
        for j in range(1, groups):
            xa_copy(j, peer(j), giver(j), peer(j)).wait_recv()

    def zs_copy(k, j):
        pos = k * per_chunk + j
        return pltpu.make_async_remote_copy(
            src_ref=slots.at[pos], dst_ref=rows.at[tp, pos], send_sem=zs_s.at[0], recv_sem=zs_r.at[k],
            device_id=(grp, expert_at(k, j), tp), device_id_type=MESH)

    def each(k, action):
        if isinstance(k, int):
            if k != 0:
                action(0)
        else:
            @pl.when(k != 0)
            def _():
                action(0)

        action(1)

    def send(k, now):
        def one(j):
            other = expert_at(k, j)
            step = by_place(other // 2, order_low.index(k), order_mid.index(k), order_high.index(k))
            higher = (ep != 0) & ((z < k) | (other == 0) | ((k == 0) & (c == 0)))
            apart = jnp.where(other == 0, nz, 0) if k == 0 else nz - k
            after = jnp.maximum(step - EARLY + (7 * apart) // 16, jnp.clip((apart - 2) // 2, 0, 4))
            before = jnp.maximum(step - EARLY - (7 * k) // 16, 0)
            leave_at = jnp.minimum(jnp.where(higher, after, before), chunks - 1)

            @pl.when(leave_at == now)
            def _():
                @pl.when(higher)
                def _():
                    pl.semaphore_wait(ready.at[other], 1)

                zs_copy(k, j).start()

        each(k, one)

    features = column[...].reshape(local_tokens, slice_width)

    by_distance = [0] + [k for i in range(1, half) for k in (i, nz - i)] + [half]
    with jax.named_scope("dispatch"):
        for k in by_distance:
            picked = jnp.dot(
                select[k * chunk_rows:(k + 1) * chunk_rows, :], features, preferred_element_type=F32)
            slots[k * per_chunk:(k + 1) * per_chunk] = picked.reshape(per_chunk, block, slice_width).astype(BF)
            send(k, 0)
    rows[tp, 0] = slots[0]

    high = gate.astype(BF).astype(F32)
    low = gate - high
    comb_hi[...] = jnp.where(chosen, high[:, None, :], zero).reshape(experts * block, local_tokens).T.astype(BF)
    comb_lo[...] = jnp.where(chosen, low[:, None, :], zero).reshape(experts * block, local_tokens).T.astype(BF)

    with jax.named_scope("weights"):
        for copy in w_copies:
            copy.wait()

    def settle(ref, sem):
        pltpu.make_async_copy(ref, ref, sem).wait()

    def span(k):
        return pl.ds(k * per_chunk, per_chunk)

    def neighbour(way):
        return peer(1) if way == 0 else peer(groups - 1)

    def move(src, dst, send, recv, k, way):
        return pltpu.make_async_remote_copy(
            src_ref=src, dst_ref=dst, send_sem=send.at[0], recv_sem=recv.at[k],
            device_id=(grp, ep, neighbour(way)), device_id_type=MESH)

    def ag_copy(k, way, owner):
        return move(rows.at[tp, span(k)], rows.at[owner, span(k)], ag_s, ag_r, k, way)

    def re_copy(k, way, src, dst):
        pos = k * per_chunk + way
        return move(rows.at[src, pos], rows.at[dst, pos], re_s, re_r, k, way)

    def ra_copy(k, way):
        pos = k * per_chunk + way
        return move(partial.at[peer(2), pos], raw.at[pos], ra_s, ra_r, k, way)

    def rs_copy(k, way):
        return move(partial.at[neighbour(way), span(k)], terms.at[way, span(k)], rs_s, rs_r, k, way)

    def zr_copy(k, j):
        pos = k * per_chunk + j
        return pltpu.make_async_remote_copy(
            src_ref=result.at[pos], dst_ref=answers.at[pos], send_sem=zr_s.at[0], recv_sem=zr_r.at[0],
            device_id=(grp, source_at(k, j), tp), device_id_type=MESH)

    def gather(k):
        with jax.named_scope("rows_wait"):
            @pl.when(k == 0)
            def _():
                settle(rows.at[tp, k * per_chunk + 1], zs_r.at[k])

            @pl.when(k != 0)
            def _():
                settle(rows.at[tp, span(k)], zs_r.at[k])

        for way in range(2):
            ag_copy(k, way, tp).start()

    def relay(k):
        with jax.named_scope("gather_wait"):
            settle(rows.at[:2, span(k)], ag_r.at[k])
        for way in range(2):
            re_copy(k, way, neighbour(1 - way), neighbour(1 - way)).start()

    def compute(k):
        with jax.named_scope("relay_wait"):
            settle(rows.at[peer(2), span(k)], re_r.at[k])
        x = jnp.concatenate(
            [rows[q, span(k)].reshape(chunk_rows, slice_width) for q in range(groups)], axis=1)
        step = 256
        for n in range(hidden_width // step):
            cols = slice(n * step, (n + 1) * step)
            g = jnp.dot(x, wg[:, cols], preferred_element_type=F32)
            u = jnp.dot(x, wu[:, cols], preferred_element_type=F32)
            hidden[:, cols] = (g * (1.0 / (1.0 + jnp.exp(-g))) * u).astype(BF)
        h = hidden[...]
        for j in (2, 1, 3, 0):
            q = peer(j)
            part = jnp.dot(
                h, wd[:, pl.ds(pl.multiple_of(q * slice_width, slice_width), slice_width)],
                preferred_element_type=F32)
            partial[q, span(k)] = part.reshape(per_chunk, block, slice_width).astype(BF)
            if j == 1:
                for way in range(2):
                    ra_copy(k, way).start()

    def forward(k):
        with jax.named_scope("raw_wait"):
            settle(raw.at[span(k)], ra_r.at[k])
        for way in range(2):
            pos = k * per_chunk + way
            both = partial[neighbour(way), pos].astype(F32) + raw[pos].astype(F32)
            partial[neighbour(way), pos] = both.astype(BF)
        for way in range(2):
            rs_copy(k, way).start()

    def give_back(k):
        with jax.named_scope("terms_wait"):
            settle(terms.at[:, span(k)], rs_r.at[k])
        total = partial[tp, span(k)].astype(F32)
        for way in range(2):
            total += terms[way, span(k)].astype(F32)
        result[span(k)] = total.astype(BF)
        each(k, lambda j: zr_copy(k, j).start())

    def pipeline(s, carry):
        @pl.when((s > 0) & (s < chunks))
        def _():
            with jax.named_scope("ready_wait"):
                for k in by_distance:
                    send(k, s)

        for lag, stage in ((6, forward), (8, give_back), (2, relay), (4, compute), (0, gather)):
            @pl.when((s >= lag) & (s < chunks + lag))
            def _(lag=lag, stage=stage):
                stage(part_at(s - lag))
        return carry

    lax.fori_loop(0, chunks + 8, pipeline, 0)
    answers[0] = result[0]

    with jax.named_scope("answers_wait"):
        settle(answers.at[:experts - 1], zr_r.at[0])
    outs = answers[...].reshape(experts * block, slice_width)
    combined = jnp.dot(comb_hi[...], outs, preferred_element_type=F32)
    combined += jnp.dot(comb_lo[...], outs, preferred_element_type=F32)

    own = jnp.sum(combined * combined, axis=1, keepdims=True)
    squares[tp] = jnp.broadcast_to(own, (local_tokens, 128)).T[:8]

    def sq_copy(j, owner):
        return pltpu.make_async_remote_copy(
            src_ref=squares.at[tp], dst_ref=squares.at[owner], send_sem=sq_s.at[j - 1], recv_sem=sq_r.at[j - 1],
            device_id=(grp, ep, peer(j)), device_id_type=MESH)

    for j in range(1, groups):
        sq_copy(j, tp).start()
    with jax.named_scope("squares_wait"):
        for j in range(1, groups):
            sq_copy(j, giver(j)).wait_recv()
    total = squares[0] + squares[1] + squares[2] + squares[3]
    scale = lax.rsqrt(total / width + EPS)
    scale = jnp.concatenate([scale] * 16, axis=0).T[:, :1]
    out_ref[...] = (combined * scale * gout_ref[...]).astype(BF)

    with jax.named_scope("drain"):
        settle(slots.at[:experts - 1], zs_s.at[0])
        settle(slots.at[:experts - 1], zr_s.at[0])
        settle(rows.at[:2], ag_s.at[0])
        settle(slots, re_s.at[0])
        settle(slots, ra_s.at[0])
        settle(terms, rs_s.at[0])
    for j in range(1, groups):
        xa_copy(j, peer(j), tp, peer(j)).wait_send()
        sq_copy(j, tp).wait_send()


def local(tokens, gain_in, routes, gates, w_gate, w_up, w_down, gain_out):
    count, width = tokens.shape
    choose = routes.shape[1]
    experts = lax.axis_size("ep")
    groups = lax.axis_size("tp")
    cap = (3 * count * choose + 2 * experts - 1) // (2 * experts)
    hidden_width = w_gate.shape[2]
    slice_width = width // groups
    block = groups * cap
    tokens_here = groups * count
    chunks = experts // 2
    vmem = pl.BlockSpec(memory_space=pltpu.VMEM)
    hbm = pl.BlockSpec(memory_space=pl.ANY)
    dma = pltpu.SemaphoreType.DMA
    return pl.pallas_call(
        functools.partial(layer_kernel, experts, groups, cap),
        out_shape=jax.ShapeDtypeStruct((tokens_here, slice_width), BF),
        in_specs=[vmem, vmem, vmem, vmem, hbm, hbm, hbm, vmem],
        out_specs=vmem,
        scratch_shapes=[
            pltpu.VMEM((width, hidden_width), BF),
            pltpu.VMEM((width, hidden_width), BF),
            pltpu.VMEM((hidden_width, width), BF),
            pltpu.VMEM((groups, count, slice_width), BF),
            pltpu.VMEM((groups, count, slice_width), BF),
            pltpu.VMEM((experts * block, tokens_here), BF),
            pltpu.VMEM((experts, block, slice_width), BF),
            pltpu.VMEM((groups, experts, block, slice_width), BF),
            pltpu.VMEM((2 * block, hidden_width), BF),
            pltpu.VMEM((groups, experts, block, slice_width), BF),
            pltpu.VMEM((experts, block, slice_width), BF),
            pltpu.VMEM((2, experts, block, slice_width), BF),
            pltpu.VMEM((experts, block, slice_width), BF),
            pltpu.VMEM((experts, block, slice_width), BF),
            pltpu.VMEM((tokens_here, experts * block), BF),
            pltpu.VMEM((tokens_here, experts * block), BF),
            pltpu.VMEM((groups, 8, tokens_here), F32),
            pltpu.SemaphoreType.REGULAR((experts,)),
            dma((3,)),
            dma((groups - 1,)), dma((groups - 1,)),
            *[dma((n,)) for n in (1, chunks) * 5],
            dma((1,)), dma((1,)),
            dma((groups - 1,)), dma((groups - 1,)),
        ],
        compiler_params=pltpu.CompilerParams(
            collective_id=0, has_side_effects=True, vmem_limit_bytes=56 * 1024 * 1024),
        name="routed_experts",
    )(tokens, gain_in.reshape(1, width), routes.T, gates.T, w_gate, w_up, w_down, gain_out.reshape(1, slice_width))


def solution(mesh):
    in_specs = (
        P(("grp", "ep", "tp"), None),
        P(),
        P(("grp", "ep"), None),
        P(("grp", "ep"), None),
        P("ep", None, "tp"),
        P("ep", None, "tp"),
        P("ep", "tp", None),
        P("tp"),
    )
    out_specs = P(("grp", "ep"), "tp")
    return jax.shard_map(local, mesh=mesh, in_specs=in_specs, out_specs=out_specs, check_vma=False)
```

```python
import functools

import jax
import jax.numpy as jnp
from jax import lax
from jax.experimental import pallas as pl
from jax.experimental.pallas import tpu as pltpu
from jax.sharding import PartitionSpec as P

EPS = 1e-06
MESH = pl.DeviceIdType.MESH
BF = jnp.bfloat16
F32 = jnp.float32
NEAR = 4
EARLY = 5


def layer_kernel(
    experts, groups, cap,
    tokens_ref, gain_ref, routes_ref, gates_ref, wg_hbm, wu_hbm, wd_hbm, gout_ref,
    out_ref,
    wg, wu, wd, piece, column, select, slots, rows, hidden, partial, raw, terms, result, answers, comb_hi, comb_lo, squares,
    ready, w_sem, xa_s, xa_r, zs_s, zs_r, ag_s, ag_r, re_s, re_r, ra_s, ra_r, rs_s, rs_r, zr_s, zr_r, sq_s, sq_r,
):
    grp, ep, tp = lax.axis_index("grp"), lax.axis_index("ep"), lax.axis_index("tp")
    z, c = ep // 2, ep % 2
    nz = experts // 2
    count, width = tokens_ref.shape
    local_tokens = groups * count
    slice_width = width // groups
    block = groups * cap
    per_chunk = 2
    chunks = experts // per_chunk
    chunk_rows = per_chunk * block
    hidden_width = wg.shape[1]

    half = nz // 2
    ends = [k for i in range(1, NEAR) for k in (nz - i, i)] + [0]
    middle = [NEAR] + [k for i in range(NEAR, half - 1) for k in (nz - i, i + 1)] + [half + 1, half]
    order_low = list(range(1, NEAR + 1)) + [0, NEAR + 1] + list(range(nz - NEAR + 1, nz)) + middle[3:] + middle[1:2]
    order_low = [k for i, k in enumerate(order_low) if k not in order_low[:i]]
    order_mid = ends + middle
    order_high = ends + middle[::-1]

    def by_place(chip, low, mid, high):
        return jnp.where(chip < NEAR, low, jnp.where(chip < half, mid, high))

    here = [by_place(z, *ks) for ks in zip(order_low, order_mid, order_high)]

    def part_at(s):
        k = here[0]
        for i in range(1, nz):
            k = jnp.where(s == i, here[i], k)
        return k

    def expert_at(k, j):
        return ((z + nz - k) % nz) * 2 + (c + j) % 2

    def source_at(k, j):
        return ((z + k) % nz) * 2 + (c + j) % 2

    rank_here = (ep + experts - 1) % experts

    def at_rank(r):
        return (r + 1) % experts

    def peer(j):
        return (tp + j) % groups

    def giver(j):
        return (tp + groups - j) % groups

    barrier = pltpu.get_barrier_semaphore()

    def signal(sem, device):
        pl.semaphore_signal(sem, inc=1, device_id=device, device_id_type=MESH)

    for j in range(1, groups):
        signal(barrier, (grp, ep, peer(j)))

    def greet(r, carry):
        signal(barrier, (grp, at_rank(r), tp))
        return carry

    lax.fori_loop(rank_here + 1, experts, greet, 0)

    w_copies = [
        pltpu.make_async_copy(src.at[0], dst, w_sem.at[i])
        for i, (src, dst) in enumerate(((wg_hbm, wg), (wu_hbm, wu), (wd_hbm, wd)))
    ]
    for copy in w_copies:
        copy.start()

    values = tokens_ref[...].astype(F32)
    normed = values * lax.rsqrt(jnp.mean(values * values, axis=-1, keepdims=True) + EPS) * gain_ref[...]
    normed = normed.astype(BF)
    for q in range(groups):
        piece[q] = normed[:, q * slice_width:(q + 1) * slice_width]

    at = lax.broadcasted_iota(jnp.int32, (experts, local_tokens), 0)
    expert = expert_at(at // per_chunk, at % per_chunk)
    hit0 = routes_ref[0:1, :] == expert
    hit1 = routes_ref[1:2, :] == expert
    zero = jnp.zeros((), F32)
    one = jnp.ones((), F32)
    hit = jnp.where(hit0, one, zero) + jnp.where(hit1, one, zero)
    before = (
        lax.broadcasted_iota(jnp.int32, (local_tokens, local_tokens), 0)
        < lax.broadcasted_iota(jnp.int32, (local_tokens, local_tokens), 1)
    )
    before = jnp.where(before, one, zero).astype(BF)
    rank = jnp.dot(hit.astype(BF), before, preferred_element_type=F32)
    rank = jnp.where(hit > 0, rank, -one)
    gate = jnp.where(hit0, gates_ref[0:1, :], zero) + jnp.where(hit1, gates_ref[1:2, :], zero)
    slot_of = lax.broadcasted_iota(jnp.int32, (experts, block, local_tokens), 1).astype(F32)
    chosen = rank[:, None, :] == slot_of
    select[...] = jnp.where(chosen, one, zero).reshape(experts * block, local_tokens).astype(BF)

    with jax.named_scope("entry"):
        pl.semaphore_wait(barrier, groups - 1 + rank_here)

    def answer(r, carry):
        signal(ready.at[ep], (grp, at_rank(r), tp))
        return carry

    lax.fori_loop(0, rank_here, answer, 0)

    def xa_copy(j, src, dst, device):
        return pltpu.make_async_remote_copy(
            src_ref=piece.at[src], dst_ref=column.at[dst], send_sem=xa_s.at[j - 1], recv_sem=xa_r.at[j - 1],
            device_id=(grp, ep, device), device_id_type=MESH)

    for j in range(1, groups):
        xa_copy(j, peer(j), tp, peer(j)).start()
    column[tp] = piece[tp]
    with jax.named_scope("slices"):
        for j in range(1, groups):
            xa_copy(j, peer(j), giver(j), peer(j)).wait_recv()

    def zs_copy(k, j):
        pos = k * per_chunk + j
        return pltpu.make_async_remote_copy(
            src_ref=slots.at[pos], dst_ref=rows.at[tp, pos], send_sem=zs_s.at[0], recv_sem=zs_r.at[k],
            device_id=(grp, expert_at(k, j), tp), device_id_type=MESH)

    def each(k, action):
        if isinstance(k, int):
            if k != 0:
                action(0)
        else:
            @pl.when(k != 0)
            def _():
                action(0)

        action(1)

    def send(k, now):
        def one(j):
            other = expert_at(k, j)
            step = by_place(other // 2, order_low.index(k), order_mid.index(k), order_high.index(k))
            higher = (ep != 0) & ((z < k) | (other == 0) | ((k == 0) & (c == 0)))
            apart = jnp.where(other == 0, nz, 0) if k == 0 else nz - k
            latest = jnp.where(other == 0, 3, 4) if 0 < k < NEAR else 4
            after = jnp.maximum(step - EARLY + (7 * apart) // 16, jnp.clip((apart - 2) // 2, 0, latest))
            before = jnp.maximum(step - EARLY - (7 * k) // 16, 0)
            leave_at = jnp.minimum(jnp.where(higher, after, before), chunks - 1)

            @pl.when(leave_at == now)
            def _():
                @pl.when(higher)
                def _():
                    pl.semaphore_wait(ready.at[other], 1)

                zs_copy(k, j).start()

        each(k, one)

    features = column[...].reshape(local_tokens, slice_width)

    by_distance = [0] + [k for i in range(1, half) for k in (i, nz - i)] + [half]
    with jax.named_scope("dispatch"):
        for k in by_distance:
            picked = jnp.dot(
                select[k * chunk_rows:(k + 1) * chunk_rows, :], features, preferred_element_type=F32)
            slots[k * per_chunk:(k + 1) * per_chunk] = picked.reshape(per_chunk, block, slice_width).astype(BF)
            send(k, 0)
    rows[tp, 0] = slots[0]

    high = gate.astype(BF).astype(F32)
    low = gate - high
    comb_hi[...] = jnp.where(chosen, high[:, None, :], zero).reshape(experts * block, local_tokens).T.astype(BF)
    comb_lo[...] = jnp.where(chosen, low[:, None, :], zero).reshape(experts * block, local_tokens).T.astype(BF)

    with jax.named_scope("weights"):
        for copy in w_copies:
            copy.wait()

    def settle(ref, sem):
        pltpu.make_async_copy(ref, ref, sem).wait()

    def span(k):
        return pl.ds(k * per_chunk, per_chunk)

    def neighbour(way):
        return peer(1) if way == 0 else peer(groups - 1)

    def move(src, dst, send, recv, k, way):
        return pltpu.make_async_remote_copy(
            src_ref=src, dst_ref=dst, send_sem=send.at[0], recv_sem=recv.at[k],
            device_id=(grp, ep, neighbour(way)), device_id_type=MESH)

    def ag_copy(k, way, owner):
        return move(rows.at[tp, span(k)], rows.at[owner, span(k)], ag_s, ag_r, k, way)

    def re_copy(k, way, src, dst):
        pos = k * per_chunk + way
        return move(rows.at[src, pos], rows.at[dst, pos], re_s, re_r, k, way)

    def ra_copy(k, way):
        pos = k * per_chunk + way
        return move(partial.at[peer(2), pos], raw.at[pos], ra_s, ra_r, k, way)

    def rs_copy(k, way):
        return move(partial.at[neighbour(way), span(k)], terms.at[way, span(k)], rs_s, rs_r, k, way)

    def zr_copy(k, j):
        pos = k * per_chunk + j
        return pltpu.make_async_remote_copy(
            src_ref=result.at[pos], dst_ref=answers.at[pos], send_sem=zr_s.at[0], recv_sem=zr_r.at[0],
            device_id=(grp, source_at(k, j), tp), device_id_type=MESH)

    def gather(k):
        with jax.named_scope("rows_wait"):
            @pl.when(k == 0)
            def _():
                settle(rows.at[tp, k * per_chunk + 1], zs_r.at[k])

            @pl.when(k != 0)
            def _():
                settle(rows.at[tp, span(k)], zs_r.at[k])

        for way in range(2):
            ag_copy(k, way, tp).start()

    def relay(k):
        with jax.named_scope("gather_wait"):
            settle(rows.at[:2, span(k)], ag_r.at[k])
        for way in range(2):
            re_copy(k, way, neighbour(1 - way), neighbour(1 - way)).start()

    def compute(k):
        with jax.named_scope("relay_wait"):
            settle(rows.at[peer(2), span(k)], re_r.at[k])
        x = jnp.concatenate(
            [rows[q, span(k)].reshape(chunk_rows, slice_width) for q in range(groups)], axis=1)
        step = 256
        for n in range(hidden_width // step):
            cols = slice(n * step, (n + 1) * step)
            g = jnp.dot(x, wg[:, cols], preferred_element_type=F32)
            u = jnp.dot(x, wu[:, cols], preferred_element_type=F32)
            hidden[:, cols] = (g * (1.0 / (1.0 + jnp.exp(-g))) * u).astype(BF)
        h = hidden[...]
        for j in (2, 1, 3, 0):
            q = peer(j)
            part = jnp.dot(
                h, wd[:, pl.ds(pl.multiple_of(q * slice_width, slice_width), slice_width)],
                preferred_element_type=F32)
            partial[q, span(k)] = part.reshape(per_chunk, block, slice_width).astype(BF)
            if j == 1:
                for way in range(2):
                    ra_copy(k, way).start()

    def forward(k):
        with jax.named_scope("raw_wait"):
            settle(raw.at[span(k)], ra_r.at[k])
        for way in range(2):
            pos = k * per_chunk + way
            both = partial[neighbour(way), pos].astype(F32) + raw[pos].astype(F32)
            partial[neighbour(way), pos] = both.astype(BF)
        for way in range(2):
            rs_copy(k, way).start()

    def give_back(k):
        with jax.named_scope("terms_wait"):
            settle(terms.at[:, span(k)], rs_r.at[k])
        total = partial[tp, span(k)].astype(F32)
        for way in range(2):
            total += terms[way, span(k)].astype(F32)
        result[span(k)] = total.astype(BF)
        each(k, lambda j: zr_copy(k, j).start())

    def pipeline(s, carry):
        @pl.when((s > 0) & (s < chunks))
        def _():
            with jax.named_scope("ready_wait"):
                for k in by_distance:
                    send(k, s)

        for lag, stage in ((6, forward), (8, give_back), (2, relay), (4, compute), (0, gather)):
            @pl.when((s >= lag) & (s < chunks + lag))
            def _(lag=lag, stage=stage):
                stage(part_at(s - lag))
        return carry

    lax.fori_loop(0, chunks + 8, pipeline, 0)
    answers[0] = result[0]

    with jax.named_scope("answers_wait"):
        settle(answers.at[:experts - 1], zr_r.at[0])
    outs = answers[...].reshape(experts * block, slice_width)
    combined = jnp.dot(comb_hi[...], outs, preferred_element_type=F32)
    combined += jnp.dot(comb_lo[...], outs, preferred_element_type=F32)

    own = jnp.sum(combined * combined, axis=1, keepdims=True)
    squares[tp] = jnp.broadcast_to(own, (local_tokens, 128)).T[:8]

    def sq_copy(j, owner):
        return pltpu.make_async_remote_copy(
            src_ref=squares.at[tp], dst_ref=squares.at[owner], send_sem=sq_s.at[j - 1], recv_sem=sq_r.at[j - 1],
            device_id=(grp, ep, peer(j)), device_id_type=MESH)

    for j in range(1, groups):
        sq_copy(j, tp).start()
    with jax.named_scope("squares_wait"):
        for j in range(1, groups):
            sq_copy(j, giver(j)).wait_recv()
    total = squares[0] + squares[1] + squares[2] + squares[3]
    scale = lax.rsqrt(total / width + EPS)
    scale = jnp.concatenate([scale] * 16, axis=0).T[:, :1]
    out_ref[...] = (combined * scale * gout_ref[...]).astype(BF)

    with jax.named_scope("drain"):
        settle(slots.at[:experts - 1], zs_s.at[0])
        settle(slots.at[:experts - 1], zr_s.at[0])
        settle(rows.at[:2], ag_s.at[0])
        settle(slots, re_s.at[0])
        settle(slots, ra_s.at[0])
        settle(terms, rs_s.at[0])
    for j in range(1, groups):
        xa_copy(j, peer(j), tp, peer(j)).wait_send()
        sq_copy(j, tp).wait_send()


def local(tokens, gain_in, routes, gates, w_gate, w_up, w_down, gain_out):
    count, width = tokens.shape
    choose = routes.shape[1]
    experts = lax.axis_size("ep")
    groups = lax.axis_size("tp")
    cap = (3 * count * choose + 2 * experts - 1) // (2 * experts)
    hidden_width = w_gate.shape[2]
    slice_width = width // groups
    block = groups * cap
    tokens_here = groups * count
    chunks = experts // 2
    vmem = pl.BlockSpec(memory_space=pltpu.VMEM)
    hbm = pl.BlockSpec(memory_space=pl.ANY)
    dma = pltpu.SemaphoreType.DMA
    return pl.pallas_call(
        functools.partial(layer_kernel, experts, groups, cap),
        out_shape=jax.ShapeDtypeStruct((tokens_here, slice_width), BF),
        in_specs=[vmem, vmem, vmem, vmem, hbm, hbm, hbm, vmem],
        out_specs=vmem,
        scratch_shapes=[
            pltpu.VMEM((width, hidden_width), BF),
            pltpu.VMEM((width, hidden_width), BF),
            pltpu.VMEM((hidden_width, width), BF),
            pltpu.VMEM((groups, count, slice_width), BF),
            pltpu.VMEM((groups, count, slice_width), BF),
            pltpu.VMEM((experts * block, tokens_here), BF),
            pltpu.VMEM((experts, block, slice_width), BF),
            pltpu.VMEM((groups, experts, block, slice_width), BF),
            pltpu.VMEM((2 * block, hidden_width), BF),
            pltpu.VMEM((groups, experts, block, slice_width), BF),
            pltpu.VMEM((experts, block, slice_width), BF),
            pltpu.VMEM((2, experts, block, slice_width), BF),
            pltpu.VMEM((experts, block, slice_width), BF),
            pltpu.VMEM((experts, block, slice_width), BF),
            pltpu.VMEM((tokens_here, experts * block), BF),
            pltpu.VMEM((tokens_here, experts * block), BF),
            pltpu.VMEM((groups, 8, tokens_here), F32),
            pltpu.SemaphoreType.REGULAR((experts,)),
            dma((3,)),
            dma((groups - 1,)), dma((groups - 1,)),
            *[dma((n,)) for n in (1, chunks) * 5],
            dma((1,)), dma((1,)),
            dma((groups - 1,)), dma((groups - 1,)),
        ],
        compiler_params=pltpu.CompilerParams(
            collective_id=0, has_side_effects=True, vmem_limit_bytes=56 * 1024 * 1024),
        name="routed_experts",
    )(tokens, gain_in.reshape(1, width), routes.T, gates.T, w_gate, w_up, w_down, gain_out.reshape(1, slice_width))


def solution(mesh):
    in_specs = (
        P(("grp", "ep", "tp"), None),
        P(),
        P(("grp", "ep"), None),
        P(("grp", "ep"), None),
        P("ep", None, "tp"),
        P("ep", None, "tp"),
        P("ep", "tp", None),
        P("tp"),
    )
    out_specs = P(("grp", "ep"), "tp")
    return jax.shard_map(local, mesh=mesh, in_specs=in_specs, out_specs=out_specs, check_vma=False)
```
